32 devices in a mesh: fs: 8 (over z, y), tp: 4 (over x, core).
Axes of the slice: x: 2, y: 2, z: 4, core: 2. Of those that a mesh axis runs over, the one named last changes fastest.
Arguments:
- later_input: bfloat16 [4096, 2048], P(('fs', 'tp')), may hold values from -6 to 6
- earlier_input: bfloat16 [4096, 2048], P('fs'), may hold values from -6 to 6
- earlier_hidden: bfloat16 [4096, 4096], P('fs', 'tp'), may hold values from -6 to 6
- cotangent: bfloat16 [4096, 2048], P('fs'), may hold values from -6 to 6
- up_weight: bfloat16 [2048, 4096], P('fs', 'tp'), may hold values from -0.125 to 0.125
- down_weight: bfloat16 [4096, 2048], P(('tp', 'fs')), may hold values from -0.09375 to 0.09375
- up_sum: float32 [2048, 4096], P('fs', 'tp'), may hold values from -4 to 4
- down_sum: float32 [4096, 2048], P(('tp', 'fs')), may hold values from -4 to 4
Outputs:
- later_output: bfloat16 [4096, 2048], P(('fs', 'tp'))
- later_hidden: bfloat16 [4096, 4096], P('fs', 'tp')
- earlier_grad: bfloat16 [4096, 2048], P(('fs', 'tp'))
- up_sum_next: float32 [2048, 4096], P('fs', 'tp')
- down_sum_next: float32 [4096, 2048], P(('tp', 'fs'))
The draws below stay inside these ranges and needn't reach their ends.
All inputs are finite; a program needn't handle non-finite values.
Results may differ from the reference program's by a relative error of at most 0.0095.
Values may be sent and summed in bfloat16 or wider, within the bound.
A program may use at most 128 MiB of HBM per device.

```python
import jax
import jax.numpy as jnp
from jax import lax

D = 2048
FF = 4096
TOKENS = 4096
N_FS = 8
N_TP = 4


def spiked(entries, key, source, target, shards_of, factor):
    owner, partner = [(jnp.arange(entries.shape[dim]) // (entries.shape[dim] // shards_of)).reshape([-1 if axis == dim else 1 for axis in range(entries.ndim)]) for dim in (source, target)]
    chosen = jax.random.permutation(key, shards_of)[partner]
    strong = (owner == chosen) | (owner == (partner + shards_of // 2) % shards_of)
    return jnp.where(strong, factor * entries, entries)


def shard_levels(key, shape, split, low, largest):
    loudness = 1.0
    for dim, blocks in split:
        heights = jax.random.uniform(jax.random.fold_in(jax.random.fold_in(key, 6), dim), (blocks,), jnp.float32, low / len(split), largest / len(split))
        loudness = loudness * jnp.repeat(jnp.exp(heights), shape[dim] // blocks).reshape((-1,) + (1,) * (len(shape) - 1 - dim))
    return loudness


def scatter_about(key, shape, deviation, reach, split=(), held_as=jnp.bfloat16):
    entries = jax.random.normal(key, shape, jnp.float32) * deviation
    if len(split) > 0:
        entries = shard_levels(key, shape, split, -0.22, 0.18) * entries
    return jnp.clip(entries, min=-reach, max=reach).astype(held_as)


def heavy_noise(own_key, shape, scale, reach, cuts, heavy, kind=jnp.bfloat16):
    array = scale * jax.random.normal(own_key, shape, jnp.float32)
    if cuts:
        array = array * shard_levels(own_key, shape, cuts, -0.22, 0.18)
    return jnp.clip(spiked(array, jax.random.fold_in(own_key, 3), *heavy), -reach, reach).astype(kind)


def setup_inputs(seed: int = 0) -> dict:
    arg_keys = jax.random.split(jax.random.key(seed), 9)
    later_input = scatter_about(arg_keys[0], (TOKENS, D), 1.0, 6.0, ((0, 32),))
    earlier_input = heavy_noise(arg_keys[1], (TOKENS, D), 1.0, 6.0, ((0, 8),), (0, 1, 8, 2.0))
    earlier_hidden = scatter_about(arg_keys[2], (TOKENS, FF), 1.0, 6.0, ((0, 8), (1, 4)))
    cotangent = heavy_noise(arg_keys[3], (TOKENS, D), 1.0, 6.0, ((0, 8),), (0, 1, 8, 2.0))
    up_weight = scatter_about(arg_keys[4], (D, FF), D ** -0.5, 0.125, ((0, 8), (1, 4)))
    down_weight = scatter_about(arg_keys[5], (FF, D), FF ** -0.5, 0.09375, ((0, 32),))
    up_sum = scatter_about(arg_keys[6], (D, FF), 0.5, 4.0, ((0, 8), (1, 4)), jnp.float32)
    down_sum = scatter_about(arg_keys[7], (FF, D), 0.5, 4.0, ((0, 32),), jnp.float32)
    return dict(later_input=later_input, earlier_input=earlier_input, earlier_hidden=earlier_hidden, cotangent=cotangent, up_weight=up_weight, down_weight=down_weight, up_sum=up_sum, down_sum=down_sum)


def squared_relu(pre_values):
    lifted = jnp.maximum(pre_values.astype(jnp.float32), 0.0)
    return lifted, lifted * lifted


def rounded_split_sum(left_rows, right_rows):
    span_width = left_rows.shape[1] // N_TP
    running = jnp.zeros((left_rows.shape[0], right_rows.shape[1]), jnp.float32)
    for block_index in range(N_TP):
        lower_edge = block_index * span_width
        upper_edge = lower_edge + span_width
        partial_value = jnp.dot(left_rows[:, lower_edge:upper_edge], right_rows[lower_edge:upper_edge],
                          preferred_element_type=jnp.float32)
        rounded = lax.optimization_barrier(partial_value.astype(jnp.bfloat16))
        running = running + rounded.astype(jnp.float32)
    return running.astype(jnp.bfloat16)


def reference(later_input, earlier_input, earlier_hidden, cotangent, up_weight, down_weight, up_sum, down_sum):
    later_hidden = jnp.dot(later_input, up_weight, preferred_element_type=jnp.float32).astype(jnp.bfloat16)
    lifted_later, squared_later = squared_relu(later_hidden)
    later_output = rounded_split_sum(squared_later.astype(jnp.bfloat16), down_weight)
    row_total = earlier_input.shape[0]
    grad_scale = float(row_total) ** -0.5
    group_rows = row_total // N_FS

    def backward_block(totals, pieces):
        inputs, hidden, upstream = pieces
        lifted, squared = squared_relu(hidden)
        activation = squared.astype(jnp.bfloat16)
        act_slope = jnp.dot(upstream, down_weight.T, preferred_element_type=jnp.float32)
        pre_grad = (2.0 * act_slope * lifted).astype(jnp.bfloat16)
        up_total = totals[0] + jnp.dot(inputs.T, pre_grad, preferred_element_type=jnp.float32)
        down_total = totals[1] + jnp.dot(activation.T, upstream, preferred_element_type=jnp.float32)
        return (up_total, down_total), rounded_split_sum(pre_grad, up_weight.T)

    stacked = (earlier_input.reshape(N_FS, group_rows, -1),
               earlier_hidden.reshape(N_FS, group_rows, -1),
               cotangent.reshape(N_FS, group_rows, -1))
    initial = (jnp.zeros(up_weight.shape, jnp.float32), jnp.zeros(down_weight.shape, jnp.float32))
    (up_total, down_total), grads = lax.scan(backward_block, initial, stacked)
    earlier_grad = grads.reshape(row_total, -1)
    return (later_output, later_hidden, earlier_grad,
            up_sum + grad_scale * up_total, down_sum + grad_scale * down_total)
```

```python
import jax
import jax.numpy as jnp
from jax import lax
from jax.sharding import PartitionSpec as P


F32, BF16 = jnp.float32, jnp.bfloat16


def contract_last(left_rows, right_rows):
    return lax.dot_general(
        left_rows, right_rows, (((1,), (1,)), ((), ())), preferred_element_type=F32
    )


def contract_first(left_rows, right_rows):
    return lax.dot_general(
        left_rows, right_rows, (((0,), (0,)), ((), ())), preferred_element_type=F32
    )


class Ring:
    def __init__(self, axis, n):
        self.axis, self.n = axis, n
        self.folded = n % 2 == 0
        if self.folded:
            self.order = [2 * p if p < n // 2 else 2 * (n - 1 - p) + 1 for p in range(n)]
        else:
            self.order = list(range(n))
        me = lax.axis_index(axis)
        self.place = self.place_of(me)

    def place_of(self, index):
        if not self.folded:
            return index
        half = lax.div(index, 2)
        return jnp.where(lax.rem(index, 2) == 0, half, self.n - 1 - half)

    def index_at(self, offset):
        p = lax.rem(self.place + (offset % self.n), self.n)
        if not self.folded:
            return p
        return jnp.where(p < self.n // 2, 2 * p, 2 * (self.n - 1 - p) + 1)

    def send(self, x, step):
        n = self.n
        perm = [(self.order[p], self.order[(p + step) % n]) for p in range(n)]
        return lax.ppermute(x, self.axis, perm)

    def schedule(self):
        n = self.n
        return n // 2, n % 2 == 0

    def gather(self, shard):
        n, rows = self.n, shard.shape[0]
        hops, cut = self.schedule()
        half = shard.shape[1] // 2
        whole = jnp.zeros((n * rows,) + shard.shape[1:], shard.dtype)

        def put(whole, block, offset, column=0):
            return lax.dynamic_update_slice(
                whole, block, (self.index_at(offset) * rows, column)
            )

        whole = put(whole, shard, 0)
        up = down = shard
        for hop in range(1, hops + 1):
            if cut and hop == hops:
                up = self.send(up[:, :half], 1)
                down = self.send(down[:, half:], -1)
                whole = put(whole, up, -hop, 0)
                whole = put(whole, down, hop, half)
            else:
                up = self.send(up, 1)
                down = self.send(down, -1)
                whole = put(whole, up, -hop)
                whole = put(whole, down, hop)
        return whole

    def scatter_sum(self, total):
        n = self.n
        rows = total.shape[0] // n
        half = total.shape[1] // 2
        hops, cut = self.schedule()

        def part(offset):
            return lax.dynamic_slice(
                total, (self.index_at(offset) * rows, 0), (rows, total.shape[1])
            )

        up = down = None
        for hop in range(hops, 0, -1):
            mine_up, mine_down = part(hop), part(-hop)
            if cut and hop == hops:
                up = self.send(mine_up[:, :half].astype(BF16), 1)
                down = self.send(mine_down[:, half:].astype(BF16), -1)
                if hop > 1:
                    up = jnp.pad(up, ((0, 0), (0, total.shape[1] - half)))
                    down = jnp.pad(down, ((0, 0), (half, 0)))
                else:
                    return part(0) + jnp.concatenate([up, down], axis=1).astype(F32)
            else:
                if up is not None:
                    mine_up = mine_up + up.astype(F32)
                    mine_down = mine_down + down.astype(F32)
                up = self.send(mine_up.astype(BF16), 1)
                down = self.send(mine_down.astype(BF16), -1)
        return part(0) + up.astype(F32) + down.astype(F32)


def rotate(x, axis, n, step):
    return lax.ppermute(x, axis, [(i, (i + step) % n) for i in range(n)])


def gather_direct(shard, axis, n):
    rows = shard.shape[0]
    me = lax.axis_index(axis)
    whole = jnp.zeros((n * rows,) + shard.shape[1:], shard.dtype)
    whole = lax.dynamic_update_slice(whole, shard, (me * rows, 0))
    for step in range(1, n):
        block = rotate(shard, axis, n, step)
        whole = lax.dynamic_update_slice(
            whole, block, (lax.rem(me + n - step, n) * rows, 0)
        )
    return whole


def scatter_direct(partial, axis, n):
    rows = partial.shape[0] // n
    me = lax.axis_index(axis)

    def part(step):
        return lax.dynamic_slice(
            partial, (lax.rem(me + step, n) * rows, 0), (rows, partial.shape[1])
        )

    total = part(0).astype(F32)
    for step in range(1, n):
        total = total + rotate(part(step), axis, n, step).astype(F32)
    return total.astype(BF16)


def build(n_fs, n_tp):
    def shards(
        later_input, earlier_input, earlier_hidden, cotangent, up_weight, down_weight, up_sum, down_sum
    ):
        ring = Ring("fs", n_fs)
        grad_scale = float(earlier_input.shape[0] * n_fs) ** (-0.5)
        down_full = ring.gather(down_weight)
        up_full = ring.gather(up_weight)
        gathered = gather_direct(later_input, "tp", n_tp)

        lifted = jnp.maximum(earlier_hidden.astype(F32), 0.0)
        activation = (lifted * lifted).astype(BF16)
        down_total = ring.scatter_sum(contract_first(activation, cotangent))

        act_slope = contract_last(cotangent, down_full)
        pre_grad = (2.0 * act_slope * lifted).astype(BF16)
        up_total = ring.scatter_sum(contract_first(earlier_input, pre_grad))

        later_hidden = jnp.dot(gathered, up_full, preferred_element_type=F32).astype(BF16)
        lifted_later = jnp.maximum(later_hidden.astype(F32), 0.0)
        act_later = (lifted_later * lifted_later).astype(BF16)
        earlier_grad = scatter_direct(
            contract_last(pre_grad, up_full).astype(BF16), "tp", n_tp
        )
        later_output = scatter_direct(
            jnp.dot(act_later, down_full, preferred_element_type=F32).astype(BF16), "tp", n_tp
        )
        return (
            later_output,
            later_hidden,
            earlier_grad,
            up_sum + grad_scale * up_total,
            down_sum + grad_scale * down_total,
        )

    return shards


def solution(mesh):
    in_specs = (
        P(("fs", "tp"), None),
        P("fs", None),
        P("fs", "tp"),
        P("fs", None),
        P("fs", "tp"),
        P(("tp", "fs"), None),
        P("fs", "tp"),
        P(("tp", "fs"), None),
    )
    out_specs = (
        P(("fs", "tp"), None),
        P("fs", "tp"),
        P(("fs", "tp"), None),
        P("fs", "tp"),
        P(("tp", "fs"), None),
    )
    shards = build(mesh.shape["fs"], mesh.shape["tp"])
    return jax.shard_map(shards, mesh=mesh, in_specs=in_specs, out_specs=out_specs, check_vma=False)
```

```python
import jax
import jax.numpy as jnp
from jax import lax
from jax.sharding import PartitionSpec as P


F32, BF16 = jnp.float32, jnp.bfloat16


def contract_last(left_rows, right_rows):
    return lax.dot_general(
        left_rows, right_rows, (((1,), (1,)), ((), ())), preferred_element_type=F32
    )


def contract_first(left_rows, right_rows):
    return lax.dot_general(
        left_rows, right_rows, (((0,), (0,)), ((), ())), preferred_element_type=F32
    )


class Ring:
    def __init__(self, axis, n):
        self.axis, self.n = axis, n
        self.folded = n % 2 == 0
        if self.folded:
            self.order = [2 * p if p < n // 2 else 2 * (n - 1 - p) + 1 for p in range(n)]
        else:
            self.order = list(range(n))
        me = lax.axis_index(axis)
        self.place = self.place_of(me)

    def place_of(self, index):
        if not self.folded:
            return index
        half = lax.div(index, 2)
        return jnp.where(lax.rem(index, 2) == 0, half, self.n - 1 - half)

    def index_at(self, offset):
        p = lax.rem(self.place + (offset % self.n), self.n)
        if not self.folded:
            return p
        return jnp.where(p < self.n // 2, 2 * p, 2 * (self.n - 1 - p) + 1)

    def send(self, x, step):
        n = self.n
        perm = [(self.order[p], self.order[(p + step) % n]) for p in range(n)]
        return lax.ppermute(x, self.axis, perm)

    def schedule(self):
        n = self.n
        return n // 2, n % 2 == 0

    def gather(self, shard):
        n, rows = self.n, shard.shape[0]
        hops, cut = self.schedule()
        half = shard.shape[1] // 2
        whole = jnp.zeros((n * rows,) + shard.shape[1:], shard.dtype)

        def put(whole, block, offset, column=0):
            return lax.dynamic_update_slice(
                whole, block, (self.index_at(offset) * rows, column)
            )

        whole = put(whole, shard, 0)
        up = down = shard
        arrivals = []
        for hop in range(1, hops + 1):
            if cut and hop == hops:
                up = self.send(up[:, :half], 1)
                down = self.send(down[:, half:], -1)
                whole = put(whole, up, -hop, 0)
                whole = put(whole, down, hop, half)
            else:
                up = self.send(up, 1)
                down = self.send(down, -1)
                whole = put(whole, up, -hop)
                whole = put(whole, down, hop)
            arrivals.append((up, down))
        return whole, arrivals

    def scatter_sum(self, total):
        n = self.n
        rows, width = total.shape[0] // n, total.shape[1]
        half = width // 2
        hops, cut = self.schedule()

        def part(offset, lo=0, size=width):
            return lax.dynamic_slice(total, (self.index_at(offset) * rows, lo), (rows, size))

        up = down = None
        for hop in range(hops, 0, -1):
            if hop == hops:
                size = half if cut else width
                up_load = part(hop, 0, size).astype(BF16)
                down_load = part(-hop, width - size, size).astype(BF16)
            else:
                mine_up, mine_down = part(hop), part(-hop)
                if cut and hop == hops - 1:
                    up = jnp.pad(up, ((0, 0), (0, width - half)))
                    down = jnp.pad(down, ((0, 0), (half, 0)))
                up_load = (mine_up + up.astype(F32)).astype(BF16)
                down_load = (mine_down + down.astype(F32)).astype(BF16)
            up_load, down_load = yield up_load, down_load
            up, down = self.send(up_load, 1), self.send(down_load, -1)
        if cut and hops == 1:
            yield part(0) + jnp.concatenate([up, down], axis=1).astype(F32)
        else:
            yield part(0) + up.astype(F32) + down.astype(F32)


def after(values, others):
    if not others:
        return values
    return lax.optimization_barrier((tuple(values), tuple(others)))[0]


def rotate(x, axis, n, step):
    return lax.ppermute(x, axis, [(i, (i + step) % n) for i in range(n)])


def gather_direct(shard, axis, n):
    rows = shard.shape[0]
    me = lax.axis_index(axis)
    whole = jnp.zeros((n * rows,) + shard.shape[1:], shard.dtype)
    whole = lax.dynamic_update_slice(whole, shard, (me * rows, 0))
    for step in range(1, n):
        block = rotate(shard, axis, n, step)
        whole = lax.dynamic_update_slice(
            whole, block, (lax.rem(me + n - step, n) * rows, 0)
        )
    return whole


def send_direct(partial, axis, n):
    rows = partial.shape[0] // n
    me = lax.axis_index(axis)

    def part(step):
        return lax.dynamic_slice(
            partial, (lax.rem(me + step, n) * rows, 0), (rows, partial.shape[1])
        )

    return [part(0)] + [rotate(part(step), axis, n, step) for step in range(1, n)]


def add_up(blocks):
    total = blocks[0].astype(F32)
    for block in blocks[1:]:
        total = total + block.astype(F32)
    return total.astype(BF16)


def build(n_fs, n_tp):
    def shards(
        later_input, earlier_input, earlier_hidden, cotangent, up_weight, down_weight, up_sum, down_sum
    ):
        ring = Ring("fs", n_fs)
        grad_scale = float(earlier_input.shape[0] * n_fs) ** (-0.5)
        down_full, down_hops = ring.gather(down_weight)
        (up_rows,) = after((up_weight,), down_hops[0])
        up_full, _ = ring.gather(up_rows)
        gathered = gather_direct(later_input, "tp", n_tp)

        lifted = jnp.maximum(earlier_hidden.astype(F32), 0.0)
        activation = (lifted * lifted).astype(BF16)
        hops = len(down_hops)
        down_sums = ring.scatter_sum(contract_first(activation, cotangent))
        loads = next(down_sums)
        for hop in range(hops):
            if hop == 1:
                loads = after(loads, down_hops[max(hops - 2, 0)])
            loads = down_sums.send(loads)
        down_total = loads

        act_slope = contract_last(cotangent, down_full)
        pre_grad = (2.0 * act_slope * lifted).astype(BF16)
        up_sums = ring.scatter_sum(contract_first(earlier_input, pre_grad))
        loads = next(up_sums)
        rows, gathered = after((pre_grad, gathered), loads)

        earlier_part = contract_last(rows, up_full).astype(BF16)
        earlier_blocks = send_direct(earlier_part, "tp", n_tp)
        loads = up_sums.send(loads)
        if hops > 1:
            (gathered,) = after((gathered,), (earlier_part,) + tuple(loads))
        later_hidden = jnp.dot(gathered, up_full, preferred_element_type=F32).astype(BF16)
        lifted_later = jnp.maximum(later_hidden.astype(F32), 0.0)
        act_later = (lifted_later * lifted_later).astype(BF16)
        later_blocks = send_direct(
            jnp.dot(act_later, down_full, preferred_element_type=F32).astype(BF16), "tp", n_tp
        )
        for hop in range(hops - 1, 0, -1):
            if hop == 1:
                loads = after(loads, earlier_blocks[1:] + later_blocks[1:])
            loads = up_sums.send(loads)
        up_total = loads
        earlier_grad, later_output = add_up(earlier_blocks), add_up(later_blocks)
        return (
            later_output,
            later_hidden,
            earlier_grad,
            up_sum + grad_scale * up_total,
            down_sum + grad_scale * down_total,
        )

    return shards


def solution(mesh):
    in_specs = (
        P(("fs", "tp"), None),
        P("fs", None),
        P("fs", "tp"),
        P("fs", None),
        P("fs", "tp"),
        P(("tp", "fs"), None),
        P("fs", "tp"),
        P(("tp", "fs"), None),
    )
    out_specs = (
        P(("fs", "tp"), None),
        P("fs", "tp"),
        P(("fs", "tp"), None),
        P("fs", "tp"),
        P(("tp", "fs"), None),
    )
    shards = build(mesh.shape["fs"], mesh.shape["tp"])
    return jax.shard_map(shards, mesh=mesh, in_specs=in_specs, out_specs=out_specs, check_vma=False)
```
